32 devices in a mesh: fs: 8 (over z, x), tp: 4 (over y, core).
Axes of the slice: x: 2, y: 2, z: 4, core: 2. Of those that a mesh axis runs over, the one named last changes fastest.
Arguments:
- layer_inputs: bfloat16 [20480, 2048], P('fs'), may hold values from -6 to 6
- output_cot: bfloat16 [20480, 2048], P('fs'), may hold values from -6 to 6
- query_cot: bfloat16 [20480, 2048], P('fs', 'tp'), may hold values from -6 to 6
- head_outputs: bfloat16 [20480, 2048], P('fs', 'tp'), may hold values from -6 to 6
- weights: float32 [2, 2048, 2048], P(None, 'fs', 'tp'), may hold values from -0.125 to 0.125
- factors: bfloat16 [2, 2048, 256], replicated, may hold values from -0.125 to 0.125
- first_moment: float32 [2, 256, 2048], P(None, None, 'tp'), may hold values from -600 to 600
- second_moment: float32 [2, 256, 2048], P(None, None, 'tp'), may hold values from 1000 to 100000
Outputs:
- new_weights: float32 [2, 2048, 2048], P(None, 'fs', 'tp')
- update: float32 [2, 2048, 2048], P(None, 'fs', 'tp')
- new_first: float32 [2, 256, 2048], P(None, None, 'tp')
- new_second: float32 [2, 256, 2048], P(None, None, 'tp')
- weight_copy: bfloat16 [2, 2048, 2048], P(None, None, 'tp')
The draws below stay inside these ranges and needn't reach their ends.
All inputs are finite; a program needn't handle non-finite values.
Results may differ from the reference program's by a relative error of at most 0.00055.
Values may be sent and summed in bfloat16 or wider, within the bound.
A program may use at most 128 MiB of HBM per device.

```python
import math
import jax
import jax.numpy as jnp
from jax import lax

D = 2048
QDIM = 2048
RANK = 256
TOKENS = 20480


def block_scale(own_key, shape, split, smallest, high):
    def one(dim, blocks):
        steps = jax.random.uniform(jax.random.fold_in(jax.random.fold_in(own_key, 6), dim), (blocks,), jnp.float32, smallest / len(split), high / len(split))
        return jnp.repeat(jnp.exp(steps), shape[dim] // blocks).reshape((-1,) + (1,) * (len(shape) - dim - 1))

    loudness = one(*split[0])
    for cut in split[1:]:
        loudness = loudness * one(*cut)
    return loudness


def noise(own_key, extent, spread, reach, cuts=(), kind=jnp.bfloat16):
    result = spread * jax.random.normal(own_key, extent, jnp.float32)
    if cuts:
        result = result * block_scale(own_key, extent, cuts, -0.22, 0.18)
    return jnp.clip(result, -reach, reach).astype(kind)


def setup_inputs(seed: int = 0) -> dict:
    streams_of = jax.random.split(jax.random.key(seed), 9)
    return {
        "layer_inputs": noise(streams_of[0], (TOKENS, D), 1.0, 6.0, ((0, 8),)),
        "output_cot": noise(streams_of[1], (TOKENS, D), 1.0, 6.0, ((0, 8),)),
        "query_cot": noise(streams_of[2], (TOKENS, QDIM), 1.0, 6.0, ((0, 8), (1, 4))),
        "head_outputs": noise(streams_of[3], (TOKENS, QDIM), 1.0, 6.0, ((0, 8), (1, 4))),
        "weights": noise(streams_of[4], (2, D, QDIM), D ** -0.5, 0.125, ((1, 8), (2, 4)), jnp.float32),
        "factors": noise(streams_of[5], (2, D, RANK), D ** -0.5, 0.125),
        "first_moment": noise(streams_of[6], (2, RANK, QDIM), 100.0, 600.0, ((2, 4),), jnp.float32),
        "second_moment": jnp.clip(jnp.exp(math.log(100000.0) - 4.6051702 * jax.random.uniform(streams_of[7], (2, RANK, QDIM), jnp.float32) ** block_scale(streams_of[7], (2, RANK, QDIM), ((2, 4),), -0.2, 0.2)), 1000.0, 100000.0),
    }


def reference(layer_inputs, output_cot, query_cot, head_outputs, weights, factors, first_moment, second_moment):
    lefts = (layer_inputs, output_cot)
    rights = (query_cot, head_outputs)
    steps = []
    firsts = []
    seconds = []
    for index in range(2):
        grad = jnp.dot(lefts[index].T, rights[index], preferred_element_type=jnp.float32)
        factor = factors[index].astype(jnp.float32)
        low = jnp.dot(factor.T, grad, precision=lax.Precision.HIGHEST)
        first = 0.9 * first_moment[index] + 0.1 * low
        second = 0.95 * second_moment[index] + 0.05 * low * low
        normed = first / (jnp.sqrt(second) + 1e-06)
        ratio = jnp.sqrt(jnp.sum(normed * normed)) / jnp.sqrt(jnp.sum(low * low) + 1e-06)
        resid = grad - jnp.dot(factor, low, precision=lax.Precision.HIGHEST)
        steps.append(jnp.dot(factor, normed, precision=lax.Precision.HIGHEST) + ratio * resid)
        firsts.append(first)
        seconds.append(second)
    step = jnp.stack(steps)
    update = step * lax.rsqrt(jnp.mean(step * step) + 1e-06)
    new_weights = weights - 0.02 * update
    return (new_weights, update, jnp.stack(firsts), jnp.stack(seconds), new_weights.astype(jnp.bfloat16))
```

```python
from functools import partial

import jax
import jax.numpy as jnp
from jax import lax
from jax.experimental import pallas as pl
from jax.experimental.pallas import tpu as pltpu
from jax.sharding import PartitionSpec as P

MESH = pl.DeviceIdType.MESH
F32 = jnp.float32
BF16 = jnp.bfloat16


def dot(a, b):
    return lax.dot_general(a, b, (((1,), (0,)), ((), ())), preferred_element_type=F32)


def dot_t(a, b):
    return lax.dot_general(a, b, (((0,), (0,)), ((), ())), preferred_element_type=F32)


def split(value):
    high = value.astype(BF16)
    return high, (value - high.astype(F32)).astype(BF16)


def kernel(
    dims,
    x0, x1, y0, y1, w_in, f_in, m1_in, m2_in,
    o_w, o_u, o_first, o_second, o_copy,
    xv, yv, fv, wv, m1, m2,
    psend, pown, xrecv, zrecv,
    lpart, lxrecv, lsum, lzrecv, low, normed, step, gather,
    tpbuf, fsbuf, ttbuf,
    in_sem, out_sem, copy_sem,
    xs, xr, zs, zr, lxs, lxr, lzs, lzr, gzs, gzr, gxs, gxr, ts, tr, fss, fsr, tts, ttr, azs, azr, axs, axr,
):
    fs, tp, X, Z, H, lead = dims
    units = 2 * Z * H
    tokens, d = xv.shape[1], xv.shape[2]
    rows, cols = wv.shape[1], wv.shape[2]
    rank = fv.shape[2]
    half = cols // H
    rank_x, rank_f = rank // X, rank // fs
    me = lax.axis_index("fs")
    mt = lax.axis_index("tp")
    z, x = me // X, me % X

    def fs_at(jz, jx):
        return lax.rem(z + jz, Z) * X + lax.rem(x + jx, X)

    def remote(src, dst, ssem, rsem, fs_to=None, tp_to=None):
        dev = {"fs": fs_to} if tp_to is None else {"tp": tp_to}
        return pltpu.make_async_remote_copy(
            src_ref=src, dst_ref=dst, send_sem=ssem, recv_sem=rsem, device_id=dev, device_id_type=MESH
        )

    loads = [
        pltpu.make_async_copy(f_in, fv, in_sem.at[0]),
        pltpu.make_async_copy(x0, xv.at[0], in_sem.at[1]),
        pltpu.make_async_copy(y0, yv.at[0], in_sem.at[2]),
        pltpu.make_async_copy(x1, xv.at[1], in_sem.at[3]),
        pltpu.make_async_copy(y1, yv.at[1], in_sem.at[4]),
        pltpu.make_async_copy(m1_in, m1, in_sem.at[5]),
        pltpu.make_async_copy(m2_in, m2, in_sem.at[6]),
        pltpu.make_async_copy(w_in, wv, in_sem.at[7]),
    ]
    for load in loads:
        load.start()

    barrier = pltpu.get_barrier_semaphore()
    for j in range(1, fs):
        pl.semaphore_signal(barrier, inc=1, device_id={"fs": lax.rem(me + j, fs)}, device_id_type=MESH)
    for j in range(1, tp):
        pl.semaphore_signal(barrier, inc=1, device_id={"tp": lax.rem(mt + j, tp)}, device_id_type=MESH)
    pl.semaphore_wait(barrier, fs - 1 + tp - 1)

    chunk = tokens // 5 if tokens % 5 == 0 and (tokens // 5) % 128 == 0 else tokens
    loads[0].wait()
    for k in range(2):
        loads[1 + 2 * k].wait()
        loads[2 + 2 * k].wait()
        lpart[k] = jnp.zeros((rank, cols), F32)

        def project(c, carry, k=k):
            at = pl.ds(pl.multiple_of(c * chunk, 128), chunk)
            high, rest = split(dot(xv[k, at, :], fv[k]))
            right = yv[k, at, :]
            lpart[k] += dot_t(high, right) + dot_t(rest, right)
            return carry

        lax.fori_loop(0, tokens // chunk, project, 0)

    def low_x(j):
        to = lax.rem(x + j, X)
        at = pl.ds(pl.multiple_of(to * rank_x, 8), rank_x)
        return remote(lpart.at[:, at, :], lxrecv.at[j - 1], lxs.at[j - 1], lxr.at[j - 1], fs_to=fs_at(0, j))

    for j in range(1, X):
        low_x(j).start()

    def x_copy(u, j):
        return remote(
            psend.at[u, j - 1], xrecv.at[u, j - 1], xs.at[u, j - 1], xr.at[u, j - 1], fs_to=fs_at(0, j)
        )

    def unit(u):
        return lax.rem(u // (2 * H) + 1, Z), (u // H) % 2, u % H

    def grads(u, carry):
        jz, k, h = unit(u)
        right = yv[k, :, pl.ds(pl.multiple_of(h * half, 128), half)]

        def block(jx):
            at = pl.ds(pl.multiple_of(fs_at(jz, jx) * rows, 128), rows)
            return dot_t(xv[k, :, at], right)

        for j in range(1, X):
            psend[u, j - 1] = block(j)

        @pl.when(u < lead)
        def _():
            for j in range(1, X):
                x_copy(u, j).start()

        pown[u] = block(0)
        return carry

    first_part = units // 2
    lax.fori_loop(0, first_part, grads, 0)

    def low_z(j):
        at = pl.ds(pl.multiple_of(lax.rem(z + j, Z) * rank_f, 8), rank_f)
        return remote(lsum.at[:, at, :], lzrecv.at[j - 1], lzs.at[j - 1], lzr.at[j - 1], fs_to=fs_at(j, 0))

    for j in range(1, X):
        low_x(j).wait()
    total = lpart[:, pl.ds(pl.multiple_of(x * rank_x, 8), rank_x), :]
    for j in range(1, X):
        total = total + lxrecv[j - 1]
    lsum[...] = total
    for j in range(1, Z):
        low_z(j).start()

    lax.fori_loop(first_part, units, grads, 0)

    def gather_z(j, offset):
        block = low.at[x, lax.rem(z + offset, Z)]
        return remote(block, block, gzs.at[j - 1], gzr.at[j - 1], fs_to=fs_at(j, 0))

    def gather_x(j, offset):
        block = low.at[lax.rem(x + offset, X)]
        return remote(block, block, gxs.at[j - 1], gxr.at[j - 1], fs_to=fs_at(0, j))

    def tp_copy(j):
        return remote(tpbuf.at[0], tpbuf.at[j], ts.at[j - 1], tr.at[j - 1], tp_to=lax.rem(mt + j, tp))

    def z_copy(u):
        jz, k, h = unit(u)
        part = u % (2 * H)
        return remote(
            pown.at[u], zrecv.at[jz - 1, part], zs.at[jz - 1, part], zr.at[jz - 1, part], fs_to=fs_at(jz, 0)
        )

    def low_own():
        for j in range(1, Z):
            low_z(j).wait()
        value = lsum[:, pl.ds(pl.multiple_of(z * rank_f, 8), rank_f), :]
        for j in range(1, Z):
            value = value + lzrecv[j - 1]
        low[x, z] = value
        for j in range(1, Z):
            gather_z(j, 0).start()

    def low_row():
        for j in range(1, Z):
            gather_z(j, 0).wait_send()
            gather_z(j, Z - j).wait_recv()
        for j in range(1, X):
            gather_x(j, 0).start()

    def moments():
        for j in range(1, X):
            gather_x(j, 0).wait_send()
            gather_x(j, X - j).wait_recv()
        loads[5].wait()
        loads[6].wait()
        for k in range(2):
            nn = jnp.zeros((rank_f, cols), F32)
            ll = jnp.zeros((rank_f, cols), F32)
            for xi in range(X):
                for zi in range(Z):
                    at = slice((xi * Z + zi) * rank_f, (xi * Z + zi + 1) * rank_f)
                    value = low[xi, zi, k]
                    first = 0.9 * m1[k, at, :] + 0.1 * value
                    second = 0.95 * m2[k, at, :] + 0.05 * value * value
                    n = first / (jnp.sqrt(second) + 1e-06)
                    m1[k, at, :] = first
                    m2[k, at, :] = second
                    normed[k, at, :] = n
                    lpart[k, at, :] = value
                    nn = nn + n * n
                    ll = ll + value * value
            tpbuf[0, 2 * k] = jnp.full((8, 128), jnp.sum(nn), F32)
            tpbuf[0, 2 * k + 1] = jnp.full((8, 128), jnp.sum(ll), F32)
        pltpu.make_async_copy(m1, o_first, out_sem.at[0]).start()
        pltpu.make_async_copy(m2, o_second, out_sem.at[1]).start()
        for j in range(1, tp):
            tp_copy(j).start()

    ratio = [None, None]

    def project_back():
        for j in range(1, tp):
            tp_copy(j).wait()
        for k in range(2):
            nn, ll = tpbuf[0, 2 * k], tpbuf[0, 2 * k + 1]
            for j in range(1, tp):
                nn = nn + tpbuf[j, 2 * k]
                ll = ll + tpbuf[j, 2 * k + 1]
            ratio[k] = (jnp.sqrt(nn) / jnp.sqrt(ll + 1e-06))[0:1, 0:1]
            high, rest = split(normed[k] - ratio[k] * lpart[k])
            own = fv[k, pl.ds(pl.multiple_of(me * rows, 8), rows), :]
            step[k] = dot(own, high) + dot(own, rest)

    def at_unit(share):
        return min(units - 1, (units * share) // 16)

    todo = [(at_unit(2), low_own), (at_unit(6), low_row), (at_unit(11), moments), (at_unit(14), project_back)]
    for u in range(units):
        for j in range(1, X):
            x_copy(u, j).wait()
            if u + lead < units:
                x_copy(u + lead, j).start()
        value = pown[u]
        for j in range(1, X):
            value = value + xrecv[u, j - 1]
        pown[u] = value
        if u < units - 2 * H:
            z_copy(u).start()
        for when, job in todo:
            if when == u:
                job()

    squares = jnp.zeros((rows, half), F32)
    for part in range(2 * H):
        k, h = part // H, part % H
        value = pown[units - 2 * H + part]
        for j in range(1, Z):
            z_copy((j - 1) * 2 * H + part).wait()
            value = value + zrecv[j - 1, part]
        at = slice(h * half, (h + 1) * half)
        value = step[k, :, at] + ratio[k] * value
        step[k, :, at] = value
        squares = squares + value * value
    fsbuf[0] = jnp.full((8, 128), jnp.sum(squares), F32)

    def fs_copy(j):
        return remote(fsbuf.at[0], fsbuf.at[j], fss.at[j - 1], fsr.at[j - 1], fs_to=lax.rem(me + j, fs))

    def tt_copy(j):
        return remote(ttbuf.at[0], ttbuf.at[j], tts.at[j - 1], ttr.at[j - 1], tp_to=lax.rem(mt + j, tp))

    for j in range(1, fs):
        fs_copy(j).start()
    total = fsbuf[0]
    for j in range(1, fs):
        fs_copy(j).wait()
        total = total + fsbuf[j]
    ttbuf[0] = total
    for j in range(1, tp):
        tt_copy(j).start()
    for j in range(1, tp):
        tt_copy(j).wait()
        total = total + ttbuf[j]
    scale = lax.rsqrt(total / (2.0 * d * cols * tp) + 1e-06)[0:1, 0:1]

    def all_z(j, k, offset):
        block = gather.at[fs_at(offset, 0), k]
        return remote(block, block, azs.at[j - 1, k], azr.at[j - 1, k], fs_to=fs_at(j, 0))

    def all_x(s, j, k, zoff, xoff):
        block = gather.at[fs_at(zoff, xoff), k]
        return remote(block, block, axs.at[s, j - 1, k], axr.at[s, j - 1, k], fs_to=fs_at(0, j))

    def put(zoff, xoff, k):
        f = fs_at(zoff, xoff)
        at = pl.ds(pl.multiple_of(f * rows, 8), rows)
        return pltpu.make_async_copy(gather.at[f, k], o_copy.at[k, at, :], copy_sem.at[zoff, xoff, k])

    loads[7].wait()
    for k in range(2):
        update = step[k] * scale
        fresh = wv[k] - 0.02 * update
        gather[me, k] = fresh.astype(BF16)
        for j in range(1, Z):
            all_z(j, k, 0).start()
        for j in range(1, X):
            all_x(0, j, k, 0, 0).start()
        step[k] = update
        wv[k] = fresh
        put(0, 0, k).start()
    outs = [
        pltpu.make_async_copy(m1, o_first, out_sem.at[0]),
        pltpu.make_async_copy(m2, o_second, out_sem.at[1]),
        pltpu.make_async_copy(wv, o_w, out_sem.at[2]),
        pltpu.make_async_copy(step, o_u, out_sem.at[3]),
    ]
    outs[2].start()
    outs[3].start()
    for s in range(1, Z):
        for k in range(2):
            all_z(s, k, Z - s).wait_recv()
            for j in range(1, X):
                all_x(s, j, k, Z - s, 0).start()
            put(Z - s, 0, k).start()
    for s in range(Z):
        for k in range(2):
            for j in range(1, X):
                all_x(s, j, k, (Z - s) % Z, X - j).wait_recv()
                put((Z - s) % Z, X - j, k).start()
    for k in range(2):
        for s in range(1, Z):
            all_z(s, k, 0).wait_send()
        for s in range(Z):
            for j in range(1, X):
                all_x(s, j, k, (Z - s) % Z, 0).wait_send()
        for zo in range(Z):
            for xo in range(X):
                put(zo, xo, k).wait()
    for out in outs:
        out.wait()


def per_device(sizes, *args):
    layer_inputs, output_cot, query_cot, head_outputs, weights, factors, first_moment, second_moment = args
    fs, tp = sizes
    X = max(1, tp // 2)
    while fs % X:
        X -= 1
    Z = fs // X
    tokens, d = layer_inputs.shape
    rows, cols = weights.shape[1:]
    rank = factors.shape[2]
    H = 2 if cols % 256 == 0 else 1
    half = cols // H
    units = 2 * Z * H
    lead = min(3, units)
    vm, dma = pltpu.VMEM, pltpu.SemaphoreType.DMA
    x1, z1, t1, f1 = max(X - 1, 1), max(Z - 1, 1), max(tp - 1, 1), max(fs - 1, 1)
    scratch = [
        vm((2, tokens, d), BF16), vm((2, tokens, cols), BF16), vm((2, d, rank), BF16),
        vm((2, rows, cols), F32), vm((2, rank, cols), F32), vm((2, rank, cols), F32),
        vm((units, x1, rows, half), F32), vm((units, rows, half), F32), vm((units, x1, rows, half), F32),
        vm((z1, 2 * H, rows, half), F32),
        vm((2, rank, cols), F32), vm((x1, 2, rank // X, cols), F32), vm((2, rank // X, cols), F32),
        vm((z1, 2, rank // fs, cols), F32), vm((X, Z, 2, rank // fs, cols), F32),
        vm((2, rank, cols), F32), vm((2, rows, cols), F32), vm((fs, 2, rows, cols), BF16),
        vm((tp, 4, 8, 128), F32), vm((fs, 8, 128), F32), vm((tp, 8, 128), F32),
        dma((8,)), dma((4,)), dma((Z, X, 2)),
        dma((units, x1)), dma((units, x1)), dma((z1, 2 * H)), dma((z1, 2 * H)),
        dma((x1,)), dma((x1,)), dma((z1,)), dma((z1,)), dma((z1,)), dma((z1,)), dma((x1,)), dma((x1,)),
        dma((t1,)), dma((t1,)), dma((f1,)), dma((f1,)), dma((t1,)), dma((t1,)),
        dma((z1, 2)), dma((z1, 2)), dma((Z, x1, 2)), dma((Z, x1, 2)),
    ]
    anywhere = pl.BlockSpec(memory_space=pl.ANY)
    return tuple(pl.pallas_call(
        partial(kernel, (fs, tp, X, Z, H, lead)),
        out_shape=(
            jax.ShapeDtypeStruct(weights.shape, F32),
            jax.ShapeDtypeStruct(weights.shape, F32),
            jax.ShapeDtypeStruct(first_moment.shape, F32),
            jax.ShapeDtypeStruct(second_moment.shape, F32),
            jax.ShapeDtypeStruct((2, d, cols), BF16),
        ),
        in_specs=[anywhere] * 8,
        out_specs=(anywhere,) * 5,
        scratch_shapes=scratch,
        compiler_params=pltpu.CompilerParams(
            collective_id=0, has_side_effects=True, vmem_limit_bytes=67043328
        ),
    )(layer_inputs, output_cot, query_cot, head_outputs, weights, factors, first_moment, second_moment))


def solution(mesh):
    return jax.shard_map(
        partial(per_device, (mesh.shape["fs"], mesh.shape["tp"])),
        mesh=mesh,
        in_specs=(
            P("fs", None),
            P("fs", None),
            P("fs", "tp"),
            P("fs", "tp"),
            P(None, "fs", "tp"),
            P(),
            P(None, None, "tp"),
            P(None, None, "tp"),
        ),
        out_specs=(
            P(None, "fs", "tp"),
            P(None, "fs", "tp"),
            P(None, None, "tp"),
            P(None, None, "tp"),
            P(None, None, "tp"),
        ),
        check_vma=False,
    )
```
